32 devices in a mesh: rep: 2 (over x), fs: 8 (over z, y), tp: 2 (over core).
Axes of the slice: x: 2, y: 2, z: 4, core: 2. Of those that a mesh axis runs over, the one named last changes fastest.
Arguments:
- tokens: bfloat16 [16384, 2048], P(('rep', 'fs', 'tp')), may hold values from -6 to 6
- mix_gain: float32 [2048], replicated, may hold values from 0.1 to 1.9
- query_weight: bfloat16 [2048, 2048], P('fs', 'tp'), may hold values from -0.125 to 0.125
- key_weight: bfloat16 [2048, 2048], P('fs', 'tp'), may hold values from -0.125 to 0.125
- value_weight: bfloat16 [2048, 2048], P('fs', 'tp'), may hold values from -0.125 to 0.125
- gate_weight: bfloat16 [2048, 2048], P('fs', 'tp'), may hold values from -0.125 to 0.125
- out_weight: bfloat16 [2048, 2048], P('fs', 'tp'), may hold values from -0.125 to 0.125
- head_gain: float32 [2048], replicated, may hold values from 0.1 to 1.9
- channel_gain: float32 [2048], replicated, may hold values from 0.1 to 1.9
- inner_gate: bfloat16 [2048, 6144], P('fs', 'tp'), may hold values from -0.125 to 0.125
- inner_lift: bfloat16 [2048, 6144], P('fs', 'tp'), may hold values from -0.125 to 0.125
- inner_down: bfloat16 [2048, 6144], P('fs', 'tp'), may hold values from -0.078125 to 0.078125
- filter_taps: float32 [3, 6144], replicated, may hold values from -3.5 to 3.5
- filter_bias: float32 [6144], replicated, may hold values from -3 to 3
Outputs:
- result: bfloat16 [16384, 2048], P(('rep', 'fs', 'tp'))
The draws below stay inside these ranges and needn't reach their ends.
All inputs are finite; a program needn't handle non-finite values.
Results may differ from the reference program's by a relative error of at most 0.017.
Values may be sent and summed in bfloat16 or wider, within the bound.
A program may use at most 128 MiB of HBM per device.

```python
import jax
import jax.numpy as jnp
from jax import lax

D = 2048
HEADS = 8
HEAD_DIM = 256
FF = 6144
SEQ = 1024
BLOCK = 128
TAPS = 3
RW = 2048
TOKENS = 16384
N_TP = 2


def block_scale(rng, dims, shards, least, largest):
    def one(axis_at, shards_of):
        draws = jax.random.uniform(jax.random.fold_in(jax.random.fold_in(rng, 6), axis_at), (shards_of,), jnp.float32, least / len(shards), largest / len(shards))
        return jnp.repeat(jnp.exp(draws), dims[axis_at] // shards_of).reshape((-1,) + (1,) * (len(dims) - axis_at - 1))

    factor_of = one(*shards[0])
    for cut in shards[1:]:
        factor_of = factor_of * one(*cut)
    return factor_of


def noise(rng, shape, spread, limit, cuts=(), held_as=jnp.bfloat16):
    result = jax.random.normal(rng, shape, jnp.float32) * spread
    if len(cuts) > 0:
        result = block_scale(rng, shape, cuts, -0.22, 0.18) * result
    return jnp.clip(result, min=-limit, max=limit).astype(held_as)


def setup_inputs(seed: int = 0) -> dict:
    key_of = jax.random.split(jax.random.key(seed), 15)
    return {
        "tokens": noise(key_of[0], (TOKENS, D), 1.0, 6.0, ((0, 32),)),
        "mix_gain": jnp.clip(1.0 + 0.18 * jax.random.normal(key_of[1], (D,), jnp.float32), 0.1, 1.9),
        "query_weight": noise(key_of[2], (D, RW), D ** -0.5, 0.125, ((0, 8), (1, 2))),
        "key_weight": noise(key_of[3], (D, RW), D ** -0.5, 0.125, ((0, 8), (1, 2))),
        "value_weight": noise(key_of[4], (D, RW), D ** -0.5, 0.125, ((0, 8), (1, 2))),
        "gate_weight": noise(key_of[5], (D, RW), D ** -0.5, 0.125, ((0, 8), (1, 2))),
        "out_weight": noise(key_of[6], (D, RW), RW ** -0.5, 0.125, ((0, 8), (1, 2))),
        "head_gain": jnp.clip(1.0 + 0.18 * jax.random.normal(key_of[7], (RW,), jnp.float32), 0.1, 1.9),
        "channel_gain": jnp.clip(1.0 + 0.18 * jax.random.normal(key_of[8], (D,), jnp.float32), 0.1, 1.9),
        "inner_gate": noise(key_of[9], (D, FF), D ** -0.5, 0.125, ((0, 8), (1, 2))),
        "inner_lift": noise(key_of[10], (D, FF), D ** -0.5, 0.125, ((0, 8), (1, 2))),
        "inner_down": noise(key_of[11], (D, FF), FF ** -0.5, 0.078125, ((0, 8), (1, 2))),
        "filter_taps": noise(key_of[12], (TAPS, FF), TAPS ** -0.5, 3.5, (), jnp.float32),
        "filter_bias": noise(key_of[13], (FF,), 0.5, 3.0, (), jnp.float32),
    }


norm_eps = 1e-06
head_eps = 1.0
rope_base = 10000.0

def rms_scale(features, gain_row):
    mean_square = lax.optimization_barrier(jnp.mean(features * features, axis=-1, keepdims=True))
    return features * lax.rsqrt(mean_square + norm_eps) * gain_row

def rotate(heads_in, positions):
    half_width = heads_in.shape[-1] // 2
    inverse = rope_base ** (-jnp.arange(half_width, dtype=jnp.float32) / half_width)
    angles = positions[:, None] * inverse[None, :]
    cosine = jnp.cos(angles)[:, None, :]
    sine_part = jnp.sin(angles)[:, None, :]
    front_half = heads_in[..., :half_width]
    back_half = heads_in[..., half_width:]
    return jnp.concatenate([front_half * cosine - back_half * sine_part, front_half * sine_part + back_half * cosine], axis=-1)

def retain(queries, key_rows, value_rows, log_gamma, span):
    full_length, head_count, head_width = queries.shape
    blocks = full_length // span
    offsets = jnp.arange(span, dtype=jnp.float32)
    distance = offsets[:, None] - offsets[None, :]
    inside_segment_decay = jnp.where(distance[None] >= 0, jnp.exp(jnp.maximum(distance, 0.0)[None] * log_gamma[:, None, None]), 0.0)
    query_decay = jnp.exp((offsets[None, :] + 1.0) * log_gamma[:, None])
    key_decay_factor = jnp.exp((span - 1.0 - offsets[None, :]) * log_gamma[:, None])
    span_decay = jnp.exp(span * log_gamma)

    def to_spans(array):
        return array.reshape(blocks, span, head_count, head_width).transpose(0, 2, 1, 3)

    def advance(carry_state, inputs):
        query_segment, key_segment, value_span = inputs
        query_wide_precision = query_segment.astype(jnp.float32)
        key_wide_precision = key_segment.astype(jnp.float32)
        value_wide_precision = value_span.astype(jnp.float32)
        attention_scores = jnp.einsum('pol,pel->poe', query_wide_precision, key_wide_precision, precision=lax.Precision.HIGHEST) * inside_segment_decay
        span_weights = attention_scores.astype(jnp.bfloat16).astype(jnp.float32)
        within_span = jnp.einsum('hnm,hme->hne', span_weights, value_wide_precision, precision=lax.Precision.HIGHEST)
        carried = jnp.einsum('hnd,hde->hne', query_wide_precision, carry_state, precision=lax.Precision.HIGHEST) * query_decay[:, :, None]
        state_update = jnp.einsum('lqc,lqu->lcu', key_wide_precision * key_decay_factor[:, :, None], value_wide_precision, precision=lax.Precision.HIGHEST)
        return (carry_state * span_decay[:, None, None] + state_update, within_span + carried)
    initial = jnp.zeros((head_count, head_width, head_width), jnp.float32)
    unused, outputs = lax.scan(advance, initial, (to_spans(queries), to_spans(key_rows), to_spans(value_rows)))
    return outputs.transpose(0, 2, 1, 3).reshape(full_length, head_count, head_width)

def project(normed, weight):
    return jnp.dot(normed, weight, preferred_element_type=jnp.float32).astype(jnp.bfloat16)

def group_sum(hidden, weight, groups):
    seq_rows, columns = hidden.shape
    part_hidden = hidden.reshape(seq_rows, groups, columns // groups).astype(jnp.float32)
    part_weight = weight.reshape(weight.shape[0], groups, columns // groups).astype(jnp.float32)
    partial_value = jnp.einsum('sgc,dgc->gsd', part_hidden, part_weight, precision=lax.Precision.HIGHEST)
    rounded = lax.optimization_barrier(partial_value.astype(jnp.bfloat16))
    return lax.optimization_barrier(jnp.sum(rounded.astype(jnp.float32), axis=0))

def reference(tokens, mix_gain, query_weight, key_weight, value_weight, gate_weight, out_weight, head_gain, channel_gain, inner_gate, inner_lift, inner_down, filter_taps, filter_bias):
    head_ids = jnp.arange(HEADS, dtype=jnp.float32)
    log_gamma = jnp.log(1.0 - 2.0 ** (-5.0 - head_ids))
    positions = jnp.arange(SEQ, dtype=jnp.float32)

    def one_sequence(seq_rows):
        normed_in = rms_scale(seq_rows.astype(jnp.float32), mix_gain).astype(jnp.bfloat16)
        queries = project(normed_in, query_weight)
        key_rows = project(normed_in, key_weight)
        value_rows = project(normed_in, value_weight)
        gate_in = project(normed_in, gate_weight)
        q_rot = (rotate(queries.astype(jnp.float32).reshape(SEQ, HEADS, HEAD_DIM), positions) * HEAD_DIM ** (-0.5)).astype(jnp.bfloat16)
        k_rot = rotate(key_rows.astype(jnp.float32).reshape(SEQ, HEADS, HEAD_DIM), positions).astype(jnp.bfloat16)
        retained = retain(q_rot, k_rot, value_rows.reshape(SEQ, HEADS, HEAD_DIM), log_gamma, BLOCK)
        mean_square = lax.optimization_barrier(jnp.mean(retained * retained, axis=-1, keepdims=True))
        head_normed = (retained * lax.rsqrt(mean_square + head_eps)).reshape(SEQ, HEADS * HEAD_DIM) * head_gain
        mixed = (jax.nn.silu(gate_in.astype(jnp.float32)) * head_normed).astype(jnp.bfloat16)
        middle = seq_rows.astype(jnp.float32) + group_sum(mixed, out_weight, N_TP)
        normed_mid = rms_scale(middle, channel_gain).astype(jnp.bfloat16)
        gate_pre = project(normed_mid, inner_gate)
        lifted = project(normed_mid, inner_lift)
        padded = jnp.pad(gate_pre.astype(jnp.float32), ((TAPS - 1, 0), (0, 0)))
        filtered = filter_bias[None, :]
        for offset in range(TAPS):
            filtered = filtered + padded[offset:offset + SEQ] * filter_taps[offset][None, :]
        hidden = (jax.nn.silu(filtered) * lifted.astype(jnp.float32)).astype(jnp.bfloat16)
        return (middle + group_sum(hidden, inner_down, N_TP)).astype(jnp.bfloat16)
    sequences = tokens.reshape(TOKENS // SEQ, SEQ, D)
    return lax.map(one_sequence, sequences).reshape(TOKENS, D)
```

```python
import jax
import jax.numpy as jnp
from jax import lax
from jax.sharding import PartitionSpec as P

HEAD_DIM = 256
BLOCK = 128
TAPS = 3


norm_eps = 1e-06
head_eps = 1.0
rope_base = 10000.0


def rms_scale(features, gain_row):
    mean_square = jnp.mean(features * features, axis=-1, keepdims=True)
    return features * lax.rsqrt(mean_square + norm_eps) * gain_row


def rotate(heads_in, positions):
    half_width = heads_in.shape[-1] // 2
    inverse = rope_base ** (-jnp.arange(half_width, dtype=jnp.float32) / half_width)
    angles = positions[:, None] * inverse[None, :]
    cosine = jnp.cos(angles)[:, None, :]
    sine_part = jnp.sin(angles)[:, None, :]
    front_half = heads_in[..., :half_width]
    back_half = heads_in[..., half_width:]
    return jnp.concatenate(
        [front_half * cosine - back_half * sine_part, front_half * sine_part + back_half * cosine],
        axis=-1,
    )


def retain(queries, key_rows, value_rows, log_gamma, span):
    full_length, head_count, head_width = queries.shape
    blocks = full_length // span
    offsets = jnp.arange(span, dtype=jnp.float32)
    distance = offsets[:, None] - offsets[None, :]
    inside_segment_decay = jnp.where(
        distance[None] >= 0,
        jnp.exp(jnp.maximum(distance, 0.0)[None] * log_gamma[:, None, None]),
        0.0,
    )
    query_decay = jnp.exp((offsets[None, :] + 1.0) * log_gamma[:, None])
    key_decay_factor = jnp.exp((span - 1.0 - offsets[None, :]) * log_gamma[:, None])
    span_decay = jnp.exp(span * log_gamma)

    def to_spans(array):
        return array.reshape(blocks, span, head_count, head_width).transpose(0, 2, 1, 3)

    def advance(carry_state, inputs):
        query_segment, key_segment, value_span = inputs
        attention_scores = (
            jnp.einsum(
                "pol,pel->poe", query_segment, key_segment, preferred_element_type=jnp.float32
            )
            * inside_segment_decay
        )
        span_weights = attention_scores.astype(jnp.bfloat16)
        within_span = jnp.einsum(
            "hnm,hme->hne", span_weights, value_span, preferred_element_type=jnp.float32
        )
        carried = (
            jnp.einsum(
                "hnd,hde->hne",
                query_segment.astype(jnp.float32),
                carry_state,
                precision=lax.Precision.HIGHEST,
            )
            * query_decay[:, :, None]
        )
        state_update = jnp.einsum(
            "lqc,lqu->lcu",
            key_segment.astype(jnp.float32) * key_decay_factor[:, :, None],
            value_span.astype(jnp.float32),
            precision=lax.Precision.HIGHEST,
        )
        return (carry_state * span_decay[:, None, None] + state_update, within_span + carried)

    initial = jnp.zeros((head_count, head_width, head_width), jnp.float32)
    unused, outputs = lax.scan(
        advance, initial, (to_spans(queries), to_spans(key_rows), to_spans(value_rows))
    )
    return outputs.transpose(0, 2, 1, 3).reshape(full_length, head_count, head_width)


def transposed_product(rows_in, weight):
    return lax.dot_general(
        rows_in, weight, (((1,), (1,)), ((), ())), preferred_element_type=jnp.float32
    )


def shift_pairs(groups, step):
    return [(source, (source + step) % groups) for source in range(groups)]


def gather_rows(rows, groups, index):
    rows_dev = rows.shape[0]
    whole = jnp.zeros((rows_dev * groups,) + rows.shape[1:], rows.dtype)
    whole = lax.dynamic_update_slice_in_dim(whole, rows, index * rows_dev, 0)
    for step in range(1, groups):
        arrived = lax.ppermute(rows, "tp", shift_pairs(groups, step))
        owner = (index - step + groups) % groups
        whole = lax.dynamic_update_slice_in_dim(whole, arrived, owner * rows_dev, 0)
    return whole


def sum_groups(partial, groups):
    total = partial.astype(jnp.float32)
    for step in range(1, groups):
        arrived = lax.ppermute(partial, "tp", shift_pairs(groups, step))
        total = total + arrived.astype(jnp.float32)
    return total


def scatter_groups(partial, groups, index):
    rows_dev = partial.shape[0] // groups
    total = lax.dynamic_slice_in_dim(partial, index * rows_dev, rows_dev, 0).astype(jnp.float32)
    for step in range(1, groups):
        target = (index + step) % groups
        leaving = lax.dynamic_slice_in_dim(partial, target * rows_dev, rows_dev, 0)
        arrived = lax.ppermute(leaving, "tp", shift_pairs(groups, step))
        total = total + arrived.astype(jnp.float32)
    return total


def shared_width(columns, unit, numerator, denominator):
    if lax.axis_size("rep") != 2:
        return 0
    return (columns // unit) * numerator // denominator * unit


def column_pieces(array, width):
    columns = array.shape[-1]
    if width == 0:
        return [array]
    rep_index = lax.axis_index("rep")
    pieces = [lax.dynamic_slice_in_dim(array, rep_index * (columns - width), width, array.ndim - 1)]
    if columns > 2 * width:
        pieces.append(array[..., width : columns - width])
    pieces.append(
        lax.dynamic_slice_in_dim(
            array, (1 - rep_index) * (columns - width), width, array.ndim - 1
        )
    )
    return pieces


def gather_weights(weights, width):
    columns = weights[0].shape[1]
    if width == 0:
        return [[lax.all_gather(weight, "fs", axis=0, tiled=True)] for weight in weights]
    rep_index = lax.axis_index("rep")
    start = rep_index * (columns - width)
    count = len(weights)

    def cut(whole):
        each = whole.shape[1] // count
        return [whole[:, order * each : (order + 1) * each] for order in range(count)]

    own = join([lax.dynamic_slice_in_dim(weight, start, width, 1) for weight in weights])
    first = lax.all_gather(own, "fs", axis=0, tiled=True)
    pieces = [cut(first)]
    if columns > 2 * width:
        common = join([weight[:, width : columns - width] for weight in weights])
        pieces.append(cut(lax.all_gather(common, "fs", axis=0, tiled=True)))
    pieces.append(cut(lax.ppermute(first, "rep", [(0, 1), (1, 0)])))
    return [list(each) for each in zip(*pieces)]


def product(rows_in, weight):
    return jnp.dot(rows_in, weight, preferred_element_type=jnp.float32).astype(jnp.bfloat16)


def join(pieces):
    return pieces[0] if len(pieces) == 1 else jnp.concatenate(pieces, axis=-1)


def shards(
    tokens,
    mix_gain,
    query_weight,
    key_weight,
    value_weight,
    gate_weight,
    out_weight,
    head_gain,
    channel_gain,
    inner_gate,
    inner_lift,
    inner_down,
    filter_taps,
    filter_bias,
):
    tp_index = lax.axis_index("tp")
    groups = lax.axis_size("tp")
    rows_dev = tokens.shape[0]
    cols_dev = query_weight.shape[1]
    hidden_dev = inner_gate.shape[1]
    heads_dev = cols_dev // HEAD_DIM
    full_length = rows_dev * groups
    head_width = shared_width(cols_dev, HEAD_DIM, 1, 2)
    hidden_width = shared_width(hidden_dev, 128, 1, 3)
    query_set, key_set = gather_weights([query_weight, key_weight], head_width)
    value_set, gate_set = gather_weights([value_weight, gate_weight], head_width)
    (out_set,) = gather_weights([out_weight], head_width)
    inner_gate_set, inner_lift_set = gather_weights([inner_gate, inner_lift], hidden_width)
    (down_set,) = gather_weights([inner_down], hidden_width)
    whole_tokens = gather_rows(tokens, groups, tp_index)
    normed_whole = lax.optimization_barrier(
        rms_scale(whole_tokens.astype(jnp.float32), mix_gain).astype(jnp.bfloat16)
    )
    queries = join([product(normed_whole, piece) for piece in query_set])
    key_rows = join([product(normed_whole, piece) for piece in key_set])
    value_rows = join([product(normed_whole, piece) for piece in value_set])
    gate_in = join([product(normed_whole, piece) for piece in gate_set])
    positions = jnp.arange(full_length, dtype=jnp.float32)
    q_rot = (
        rotate(queries.astype(jnp.float32).reshape(full_length, heads_dev, HEAD_DIM), positions)
        * HEAD_DIM ** (-0.5)
    ).astype(jnp.bfloat16)
    k_rot = rotate(
        key_rows.astype(jnp.float32).reshape(full_length, heads_dev, HEAD_DIM), positions
    ).astype(jnp.bfloat16)
    head_order = join(
        column_pieces(jnp.arange(heads_dev, dtype=jnp.int32), head_width // HEAD_DIM)
    )
    head_ids = (tp_index * heads_dev + head_order).astype(jnp.float32)
    log_gamma = jnp.log(1.0 - 2.0 ** (-5.0 - head_ids))
    retained = retain(
        q_rot, k_rot, value_rows.reshape(full_length, heads_dev, HEAD_DIM), log_gamma, BLOCK
    )
    mean_square = jnp.mean(retained * retained, axis=-1, keepdims=True)
    gain_dev = lax.dynamic_slice_in_dim(head_gain, tp_index * cols_dev, cols_dev, 0)
    gain_dev = join(column_pieces(gain_dev, head_width))
    head_normed = (retained * lax.rsqrt(mean_square + head_eps)).reshape(
        full_length, cols_dev
    ) * gain_dev
    mixed = (jax.nn.silu(gate_in.astype(jnp.float32)) * head_normed).astype(jnp.bfloat16)
    out_product = 0.0
    column = 0
    for piece in out_set:
        part = mixed[:, column : column + piece.shape[1]]
        out_product = out_product + transposed_product(part, piece)
        column += piece.shape[1]
    mixer_whole = sum_groups(out_product.astype(jnp.bfloat16), groups)
    middle_whole = whole_tokens.astype(jnp.float32) + mixer_whole
    normed_mid = lax.optimization_barrier(
        rms_scale(middle_whole, channel_gain).astype(jnp.bfloat16)
    )
    middle = lax.dynamic_slice_in_dim(middle_whole, tp_index * rows_dev, rows_dev, 0)
    taps_dev = lax.dynamic_slice_in_dim(filter_taps, tp_index * hidden_dev, hidden_dev, 1)
    bias_dev = lax.dynamic_slice_in_dim(filter_bias, tp_index * hidden_dev, hidden_dev, 0)
    taps_set = column_pieces(taps_dev, hidden_width)
    bias_set = column_pieces(bias_dev, hidden_width)
    down_product = 0.0
    for gate_piece, lift_piece, down_piece, taps_piece, bias_piece in zip(
        inner_gate_set, inner_lift_set, down_set, taps_set, bias_set
    ):
        gate_pre = product(normed_mid, gate_piece)
        lifted = product(normed_mid, lift_piece)
        padded = jnp.pad(gate_pre, ((TAPS - 1, 0), (0, 0)))
        filtered = bias_piece[None, :]
        for offset in range(TAPS):
            shifted = padded[offset : offset + full_length].astype(jnp.float32)
            filtered = filtered + shifted * taps_piece[offset][None, :]
        hidden = (jax.nn.silu(filtered) * lifted.astype(jnp.float32)).astype(jnp.bfloat16)
        down_product = down_product + transposed_product(hidden, down_piece)
    outcome = middle + scatter_groups(down_product.astype(jnp.bfloat16), groups, tp_index)
    return outcome.astype(jnp.bfloat16)


def solution(mesh):
    in_specs = (
        P(("rep", "fs", "tp"), None),
        P(),
        P("fs", "tp"),
        P("fs", "tp"),
        P("fs", "tp"),
        P("fs", "tp"),
        P("fs", "tp"),
        P(),
        P(),
        P("fs", "tp"),
        P("fs", "tp"),
        P("fs", "tp"),
        P(),
        P(),
    )
    out_specs = P(("rep", "fs", "tp"), None)
    return jax.shard_map(shards, mesh=mesh, in_specs=in_specs, out_specs=out_specs, check_vma=False)
```
